32 devices in a mesh: ep: 4 (over z), tp: 8 (over y, x, core).
Axes of the slice: x: 2, y: 2, z: 4, core: 2. Of those that a mesh axis runs over, the one named last changes fastest.
Arguments:
- tokens: bfloat16 [32, 4096], P('ep'), may hold values from -6 to 6
- norm_gains: float32 [4, 4096], replicated, may hold values from 0.1 to 1.9
- w_query: bfloat16 [4096, 4096], P(None, 'tp'), may hold values from -0.09375 to 0.09375
- w_query_rope: bfloat16 [4096, 2048], P(None, 'tp'), may hold values from -0.09375 to 0.09375
- w_key_up: bfloat16 [32, 128, 1024], P('tp'), may hold values from -0.5 to 0.5
- w_value_up: bfloat16 [32, 1024, 128], P('tp'), may hold values from -0.1875 to 0.1875
- w_output: bfloat16 [4096, 4096], P('tp'), may hold values from -0.09375 to 0.09375
- w_latent_down: bfloat16 [4096, 1024], P(None, 'tp'), may hold values from -0.09375 to 0.09375
- latent_gain: float32 [1024], replicated, may hold values from 0.1 to 1.9
- w_rope_down: bfloat16 [4096, 64], replicated, may hold values from -0.09375 to 0.09375
- cache_latent: bfloat16 [32, 1024, 1024], P(('ep', 'tp')), may hold values from -300 to 300
- cache_rope: bfloat16 [32, 1024, 64], P(('ep', 'tp')), may hold values from -6 to 6
- lengths: int32 [32], P(('ep', 'tp')), may hold values from 1 to 1024, as said below
- routes: int32 [32, 2], P('ep'), may hold values from 0 to 3, all different within a row; in each aligned block of 8 rows (0 to 7, 8 to 15, ...) at most 7 rows name the same one
- route_weights: float32 [32, 2], P('ep'), may hold values from 0.2 to 1
- w_gate: bfloat16 [4, 4096, 2048], P('ep', None, 'tp'), may hold values from -0.09375 to 0.09375
- w_up: bfloat16 [4, 4096, 2048], P('ep', None, 'tp'), may hold values from -0.09375 to 0.09375
- w_down: bfloat16 [4, 2048, 4096], P('ep', 'tp'), may hold values from -0.125 to 0.125
Outputs:
- hidden_out: bfloat16 [32, 4096], P(('ep', 'tp'))
- new_latent: bfloat16 [32, 1024], P(('ep', 'tp'))
- new_rope: bfloat16 [32, 64], P(('ep', 'tp'))
The draws below stay inside these ranges and needn't reach their ends.
Inputs may be any that keep to these rules, and one draw needn't show every extreme that they name: `routes`: within each aligned block of 8 rows no expert is named by more than 7 rows, a bound that some block reaches; the 2 experts of a row differ. The new token stands at position lengths; some sequence has exactly 1024.
All inputs are finite; a program needn't handle non-finite values.
Results may differ from the reference program's by a relative error of at most 0.02.
Values may be sent and summed in bfloat16 or wider, within the bound.
A program may use at most 64 MiB of HBM per device.

```python
import math
import jax
import jax.numpy as jnp
import numpy as np
from jax import lax

D = 4096
HEADS = 32
NOPE = 128
ROPE = 64
VDIM = 128
LATENT = 1024
FF = 2048
TOPK = 2
EXP_LOCAL = 1
CACHE = 1024
EXPERTS = 4
GROUP_ROWS = 8
TOKENS = 32
CAP = 7
FF_DEV = 256
N_EP = 4


def draw_cache_latent(key, part):
    base_key = jax.random.fold_in(jax.random.fold_in(key, 11), 0)
    drawn = jnp.clip(jax.random.normal(base_key, (TOKENS, CACHE, LATENT), jnp.float32), -6.0, 6.0)
    return drawn.astype(jnp.bfloat16)


def draw_lengths(key, part):
    value_key, place_key = jax.random.split(jax.random.fold_in(key, 13))
    drawn = jax.random.randint(value_key, (TOKENS,), 1, CACHE + 1)
    longest = jax.random.randint(place_key, (), 0, TOKENS)
    return jnp.where(jnp.arange(TOKENS) == longest, CACHE, drawn).astype(jnp.int32)


def block_levels(key, extent, cuts, least, high):
    gain = 1.0
    for dim, blocks in cuts:
        steps = jax.random.uniform(jax.random.fold_in(jax.random.fold_in(key, 6), dim), (blocks,), jnp.float32, least / len(cuts), high / len(cuts))
        gain = gain * jnp.repeat(jnp.exp(steps), extent[dim] // blocks).reshape((-1,) + (1,) * (len(extent) - 1 - dim))
    return gain


def shared_out(stream_key, own, number, rows, count, top, reach, lean):
    sequence = jax.random.permutation(stream_key, count)
    crowded, ordinary = load_shares(count, rows * top, reach, lean, True), load_shares(count, rows * top, reach, lean, False)
    places = jnp.arange(count)

    def named(sizes, rotation):
        used = int((sizes > 0).sum())
        fixed = max(1, used // 4)
        shifted = fixed + (places - fixed + rotation * (used - fixed)) % max(1, count - fixed)
        return jnp.zeros((count,), jnp.int32).at[sequence[jnp.where(places < fixed, places, shifted)]].set(jnp.asarray(sizes, jnp.int32))

    sizes = jnp.where(number % 4 == 0, named(crowded, number // 4), named(ordinary, number - number // 4 - 1))
    mixed = jax.random.permutation(jax.random.fold_in(own, 3), count)
    source_of, receiver = mixed[0:count // 2 * 2:2], mixed[1:count // 2 * 2:2]
    slack = jnp.minimum(sizes[source_of] - 1, reach - sizes[receiver]) // 2
    slack = jnp.where((source_of == sequence[0]) | (receiver == sequence[0]) | (sizes[receiver] == 0), 0, jnp.maximum(slack, 0))
    shifted = jax.random.randint(jax.random.fold_in(own, 4), (count // 2,), 0, 1 << 20) % (slack + 1)
    sizes = sizes.at[source_of].add(-shifted).at[receiver].add(shifted)
    items = jnp.searchsorted(jnp.cumsum(sizes), jnp.arange(rows * top), side="right").astype(jnp.int32)
    table = items.reshape(top, rows).T
    table = table[jax.random.permutation(jax.random.fold_in(own, 1), rows)]
    rotation = jax.random.randint(jax.random.fold_in(own, 2), (rows, 1), 0, top)
    return jnp.take_along_axis(table, (jnp.arange(top)[None, :] + rotation) % top, axis=1)


def load_shares(number_of, total, bound, skew, full):
    loads = [(1 << 20) // math.isqrt(grade ** skew) + 1 for grade in range(1, number_of + 1)]
    largest = bound if full else min(bound, max(-(-total // number_of), total * loads[0] // sum(loads)))
    least = 1 if total - largest >= number_of - 1 else 0
    counts, rest = [largest] + [least] * (number_of - 1), total - largest - least * (number_of - 1)
    while rest > 0:
        movable = [i for i in range(1, number_of) if counts[i] < largest] or [i for i in range(1, number_of) if counts[i] < bound]
        mass, remaining = sum([loads[i] for i in movable]), rest
        for i in movable:
            addition = min(bound - counts[i], max(1, remaining * loads[i] // mass), rest)
            counts[i] = counts[i] + addition
            rest = rest - addition
    return np.array(counts)


def normal_values(stream_key, shape, scale, bound, pieces=(), kind=jnp.bfloat16):
    values = jax.random.normal(stream_key, shape, jnp.float32) * scale
    if len(pieces) > 0:
        values = block_levels(stream_key, shape, pieces, -0.22, 0.18) * values
    return jnp.clip(values, min=-bound, max=bound).astype(kind)


def setup_inputs(seed: int = 0) -> dict:
    seeds = jax.random.split(jax.random.key(seed), 19)
    tokens = normal_values(seeds[0], (TOKENS, D), 1.0, 6.0, ((0, 4),))
    norm_gains = jnp.clip(1.0 + 0.18 * jax.random.normal(seeds[1], (4, D), jnp.float32), 0.1, 1.9)
    w_query = normal_values(seeds[2], (D, HEADS * NOPE), D ** -0.5, 0.09375, ((1, 8),))
    w_query_rope = normal_values(seeds[3], (D, HEADS * ROPE), D ** -0.5, 0.09375, ((1, 8),))
    w_key_up = normal_values(seeds[4], (HEADS, NOPE, LATENT), NOPE ** -0.5, 0.5, ((0, 8),))
    w_value_up = normal_values(seeds[5], (HEADS, LATENT, VDIM), LATENT ** -0.5, 0.1875, ((0, 8),))
    w_output = normal_values(seeds[6], (HEADS * VDIM, D), (HEADS * VDIM) ** -0.5, 0.09375, ((0, 8),))
    w_latent_down = normal_values(seeds[7], (D, LATENT), D ** -0.5, 0.09375, ((1, 8),))
    latent_gain = jnp.clip(1.0 + 0.18 * jax.random.normal(seeds[8], (LATENT,), jnp.float32), 0.1, 1.9)
    w_rope_down = normal_values(seeds[9], (D, ROPE), D ** -0.5, 0.09375)
    cache_latent = draw_cache_latent(jax.random.fold_in(seeds[18], 71), 0)
    cache_rope = normal_values(seeds[11], (TOKENS, CACHE, ROPE), 1.0, 6.0, ((0, 32),))
    lengths = draw_lengths(jax.random.fold_in(seeds[18], 71), 0)
    routes_keys = jax.random.split(jax.random.fold_in(seeds[13], 1), TOKENS // GROUP_ROWS)
    routes_turns = jax.random.permutation(jax.random.fold_in(seeds[13], 3), TOKENS // GROUP_ROWS)
    routes = jax.vmap(lambda own, number: shared_out(jax.random.fold_in(seeds[13], 2), own, number, GROUP_ROWS, EXPERTS, TOPK, CAP, 2))(routes_keys, routes_turns).reshape((TOKENS, TOPK))
    route_weights = jnp.clip(0.2 + 0.8 * jax.random.uniform(seeds[14], (TOKENS, TOPK), jnp.float32) ** block_levels(seeds[14], (TOKENS, TOPK), ((0, 4),), -0.2, 0.2), 0.2, 1.0)
    w_gate = normal_values(seeds[15], (EXPERTS // EXP_LOCAL, D, EXP_LOCAL * FF), D ** -0.5, 0.09375, ((0, 4), (2, 8)))
    w_up = normal_values(seeds[16], (EXPERTS // EXP_LOCAL, D, EXP_LOCAL * FF), D ** -0.5, 0.09375, ((0, 4), (2, 8)))
    w_down = normal_values(seeds[17], (EXPERTS // EXP_LOCAL, EXP_LOCAL * FF, D), FF ** -0.5, 0.125, ((0, 4), (1, 8)))
    return dict(tokens=tokens, norm_gains=norm_gains, w_query=w_query, w_query_rope=w_query_rope, w_key_up=w_key_up, w_value_up=w_value_up, w_output=w_output, w_latent_down=w_latent_down, latent_gain=latent_gain, w_rope_down=w_rope_down, cache_latent=cache_latent, cache_rope=cache_rope, lengths=lengths, routes=routes, route_weights=route_weights, w_gate=w_gate, w_up=w_up, w_down=w_down)


EPSILON = 1e-06
ROTARY_BASE = 500000.0

def rms_scale(source, gain_row):
    values_f = source.astype(jnp.float32)
    return values_f * lax.rsqrt(lax.optimization_barrier(jnp.mean(values_f * values_f, axis=-1, keepdims=True)) + EPSILON) * gain_row.astype(jnp.float32)

def rotate(source, position):
    half_width = source.shape[-1] // 2
    frequency = ROTARY_BASE ** (-jnp.arange(half_width, dtype=jnp.float32) / half_width)
    angles = position[..., None] * frequency
    first_half = source[..., :half_width]
    second_half = source[..., half_width:]
    return jnp.concatenate([first_half * jnp.cos(angles) - second_half * jnp.sin(angles), second_half * jnp.cos(angles) + first_half * jnp.sin(angles)], axis=-1)

def attend_one(items):
    q_latent, q_pe, cache_lat, cache_rp, lat_new, rope_new, length = items
    score_scale = (NOPE + ROPE) ** (-0.5)
    scores = (jnp.einsum('hc,pc->hp', q_latent.astype(jnp.float32), cache_lat.astype(jnp.float32)) + jnp.einsum('hr,pr->hp', q_pe.astype(jnp.float32), cache_rp.astype(jnp.float32))) * score_scale
    own_score = (jnp.einsum('hc,c->h', q_latent.astype(jnp.float32), lat_new.astype(jnp.float32)) + jnp.einsum('hr,r->h', q_pe.astype(jnp.float32), rope_new.astype(jnp.float32))) * score_scale
    visible = (jnp.arange(CACHE, dtype=jnp.int32) < length)[None, :]
    row_max = jnp.maximum(lax.optimization_barrier(jnp.max(jnp.where(visible, scores, -jnp.inf), axis=-1)), own_score)
    weights = jnp.where(visible, jnp.exp(scores - row_max[:, None]), 0.0)
    own_weight = jnp.exp(own_score - row_max)
    denominator = lax.optimization_barrier(jnp.sum(weights, axis=-1)) + own_weight
    probabilities = (weights / denominator[:, None]).astype(jnp.bfloat16)
    own_prob = (own_weight / denominator).astype(jnp.bfloat16)
    attended = jnp.einsum('hp,pc->hc', probabilities.astype(jnp.float32), cache_lat.astype(jnp.float32))
    attended = attended + own_prob.astype(jnp.float32)[:, None] * lat_new.astype(jnp.float32)[None, :]
    return attended.astype(jnp.bfloat16)

def expert_total(expert_in, routes, route_weights, w_gate, w_up, w_down):
    slot_count = N_EP * CAP
    block_count = FF // FF_DEV

    def one_expert(running, expert):
        holder = (expert // EXP_LOCAL).astype(jnp.int32)
        offset = (expert % EXP_LOCAL * FF).astype(jnp.int32)
        gate_cols = lax.dynamic_slice_in_dim(w_gate[holder], offset, FF, 1)
        up_cols = lax.dynamic_slice_in_dim(w_up[holder], offset, FF, 1)
        down_rows = lax.dynamic_slice_in_dim(w_down[holder], offset, FF, 0)
        hit_mask = routes == expert
        chosen = jnp.any(hit_mask, axis=-1)
        route_weight = lax.optimization_barrier(jnp.sum(jnp.where(hit_mask, route_weights, 0.0), axis=-1))
        slot_place = (jnp.cumsum(chosen.astype(jnp.int32)) - 1).astype(jnp.int32)
        slot_target = jnp.where(chosen, slot_place, slot_count).astype(jnp.int32)
        row_index = jnp.zeros((slot_count,), jnp.int32).at[slot_target].set(jnp.arange(TOKENS, dtype=jnp.int32), mode='drop')
        expert_rows = expert_in[row_index]
        gate_sum = jnp.dot(expert_rows, gate_cols, preferred_element_type=jnp.float32)
        up_sum = jnp.dot(expert_rows, up_cols, preferred_element_type=jnp.float32)
        hidden_units = (jax.nn.silu(gate_sum) * up_sum).astype(jnp.bfloat16)
        blocks = jnp.einsum('nbf,bfd->nbd', hidden_units.reshape(slot_count, block_count, FF_DEV).astype(jnp.float32), down_rows.reshape(block_count, FF_DEV, D).astype(jnp.float32)).astype(jnp.bfloat16)
        block_sum = lax.optimization_barrier(jnp.sum(blocks.astype(jnp.float32), axis=1))
        picked = block_sum[jnp.clip(slot_place, 0, slot_count - 1).astype(jnp.int32)]
        return (running + jnp.where(chosen[:, None], route_weight[:, None] * picked, 0.0), None)
    start = jnp.zeros((TOKENS, D), jnp.float32)
    return lax.scan(one_expert, start, jnp.arange(EXPERTS, dtype=jnp.int32))[0]

def reference(tokens, norm_gains, w_query, w_query_rope, w_key_up, w_value_up, w_output, w_latent_down, latent_gain, w_rope_down, cache_latent, cache_rope, lengths, routes, route_weights, w_gate, w_up, w_down):
    normed = rms_scale(tokens, norm_gains[0]).astype(jnp.bfloat16)
    q_nope = jnp.dot(normed, w_query, preferred_element_type=jnp.float32).astype(jnp.bfloat16).reshape(TOKENS, HEADS, NOPE)
    q_latent = jnp.einsum('thn,hnc->thc', q_nope.astype(jnp.float32), w_key_up.astype(jnp.float32)).astype(jnp.bfloat16)
    q_rot = jnp.dot(normed, w_query_rope, preferred_element_type=jnp.float32).astype(jnp.bfloat16).reshape(TOKENS, HEADS, ROPE)
    latent_raw = jnp.dot(normed, w_latent_down, preferred_element_type=jnp.float32).astype(jnp.bfloat16)
    rope_raw = jnp.dot(normed, w_rope_down, preferred_element_type=jnp.float32).astype(jnp.bfloat16)
    new_latent = rms_scale(latent_raw, latent_gain).astype(jnp.bfloat16)
    position = lengths.astype(jnp.float32)
    new_rope = rotate(rope_raw.astype(jnp.float32), position).astype(jnp.bfloat16)
    q_pe = rotate(q_rot.astype(jnp.float32), position[:, None]).astype(jnp.bfloat16)
    attended = lax.map(attend_one, (q_latent, q_pe, cache_latent, cache_rope, new_latent, new_rope, lengths))
    values = jnp.einsum('thc,hcv->thv', attended.astype(jnp.float32), w_value_up.astype(jnp.float32)).astype(jnp.bfloat16)
    mixed = jnp.dot(values.reshape(TOKENS, HEADS * VDIM), w_output, preferred_element_type=jnp.float32)
    resid = (tokens.astype(jnp.float32) + rms_scale(mixed, norm_gains[1])).astype(jnp.bfloat16)
    expert_in = rms_scale(resid, norm_gains[2]).astype(jnp.bfloat16)
    routed = expert_total(expert_in, routes, route_weights, w_gate, w_up, w_down)
    hidden_out = (resid.astype(jnp.float32) + rms_scale(routed, norm_gains[3])).astype(jnp.bfloat16)
    return (hidden_out, new_latent, new_rope)
```

```python
import functools
import jax
import jax.numpy as jnp
from jax import lax
from jax.experimental import pallas as pl
from jax.experimental.pallas import tpu as pltpu
from jax.sharding import PartitionSpec as P

EPSILON = 1e-06
ROTARY_BASE = 500000.0
LANES = 128
FOLD = 8
SPLIT = 4
F32 = jnp.float32
BF16 = jnp.bfloat16


def round_up(value, step):
    return (value + step - 1) // step * step


def inv_rms(v):
    return lax.rsqrt(jnp.mean(v * v, axis=-1, keepdims=True) + EPSILON)


def folded_inv_rms(v):
    lanes = jnp.sum(v * v, axis=0, keepdims=True)
    mean = jnp.sum(lanes, axis=1, keepdims=True) / (v.shape[0] * v.shape[1])
    return lax.rsqrt(mean + EPSILON)


def fold(dst, row):
    width = row.shape[1] // FOLD
    for j in range(FOLD):
        dst[j : j + 1, :] = row[:, j * width : (j + 1) * width]


def layer_kernel(
    len_ref,
    routes_ref,
    weights_ref,
    *refs,
):
    hbm = refs[:15]
    hidden_ref, latent_out_ref, rope_out_ref = refs[15:18]
    vm = refs[18:33]
    (
        nrm,
        rot_scr,
        qs_f,
        qs,
        qrx,
        q_f,
        lat_f,
        sc_scr,
        att_f,
        as_,
        arx,
        st,
        val,
        ms,
        mrx,
        tok_row,
        es,
        erx,
        xs_f,
        xs,
        xrx,
        x_f,
        x_b,
        ys,
        yrx,
        rs,
        rrx,
        ms_f,
        gain_f,
        out_row,
        tot_f,
        load_sem,
        part_sem,
        s1,
        r1,
        s2,
        r2,
        s3,
        r3,
        s4,
        r4,
        s5,
        r5,
        s6,
        r6,
        s7,
        r7,
    ) = refs[33:]
    tok, gains, wq, wku, wqr, wld, wrd, lgain, cl, cr, wvu, wo, wg, wu, wd = vm
    T = lax.axis_size("tp")
    E = lax.axis_size("ep")
    me = lax.axis_index("tp")
    grp = lax.axis_index("ep")
    G, D = tok.shape
    H, N, C = wku.shape
    V = wvu.shape[2]
    R = wrd.shape[0]
    CC = wld.shape[1]
    POS = cl.shape[1]
    half = R // 2
    NT = (((1,), (1,)), ((), ()))

    barrier = pltpu.get_barrier_semaphore()

    def greet_tp(i, carry):
        pl.semaphore_signal(
            barrier,
            inc=1,
            device_id={"tp": lax.rem(me + i, T)},
            device_id_type=pl.DeviceIdType.MESH,
        )
        return carry

    def greet_ep(i, carry):
        pl.semaphore_signal(
            barrier,
            inc=1,
            device_id={"ep": lax.rem(grp + i, E)},
            device_id_type=pl.DeviceIdType.MESH,
        )
        return carry

    lax.fori_loop(1, T, greet_tp, 0)
    lax.fori_loop(1, E, greet_ep, 0)

    loads = [pltpu.make_async_copy(hbm[i], vm[i], load_sem.at[i]) for i in range(15)]
    part = D // SPLIT

    def projection_loads(k):
        at = pl.ds(k * part, part)
        return [
            pltpu.make_async_copy(hbm[i].at[at], vm[i].at[at], part_sem.at[i, k])
            for i in (2, 4, 5)
        ]

    for i in (0, 1):
        loads[i].start()
    for k in range(SPLIT):
        for copy in projection_loads(k):
            copy.start()
    for i in (3, 6, 7):
        loads[i].start()
    names = (
        ("tok", "gains", "wq", "wku", "wqr", "wld", "wrd", "lgain")
        + ("cl", "cr", "wvu", "wo", "wg", "wu", "wd")
    )

    def ready(*which):
        for name in which:
            loads[names.index(name)].wait()

    def rdma(axis, src, dst, send, recv, peer):
        return pltpu.make_async_remote_copy(
            src_ref=src,
            dst_ref=dst,
            send_sem=send,
            recv_sem=recv,
            device_id={axis: peer},
            device_id_type=pl.DeviceIdType.MESH,
        )

    def scatter(axis, mine, size, src, dst, send, recv):
        def pick(peer):
            return src.at[peer] if len(src.shape) == len(dst.shape) else src

        def go(i, carry):
            peer = lax.rem(mine + i, size)
            rdma(axis, pick(peer), dst.at[mine], send.at[peer], recv.at[mine], peer).start()
            return carry

        lax.fori_loop(1, size, go, 0)

    def collect(axis, mine, size, src, dst, send, recv):
        def pick(peer):
            return src.at[peer] if len(src.shape) == len(dst.shape) else src

        def go(i, carry):
            peer = lax.rem(mine + i, size)
            copy = rdma(axis, pick(peer), dst.at[peer], send.at[peer], recv.at[peer], peer)
            copy.wait_recv()
            return carry

        lax.fori_loop(1, size, go, 0)

    def drain(axis, mine, size, src, dst, send, recv):
        def pick(peer):
            return src.at[peer] if len(src.shape) == len(dst.shape) else src

        def go(i, carry):
            peer = lax.rem(mine + i, size)
            copy = rdma(axis, pick(peer), dst.at[peer], send.at[peer], recv.at[peer], peer)
            copy.wait_send()
            return carry

        lax.fori_loop(1, size, go, 0)

    def mm_k(x_ref, w_ref, width):
        chunk = min(1024, x_ref.shape[1])

        def step(k, acc):
            at = pl.ds(pl.multiple_of(k * chunk, chunk), chunk)
            return acc + jnp.dot(x_ref[:, at], w_ref[at, :], preferred_element_type=F32)

        return lax.fori_loop(
            0, x_ref.shape[1] // chunk, step, jnp.zeros((x_ref.shape[0], width), F32)
        )

    qs_f[...] = jnp.zeros_like(qs_f)
    rot_scr[...] = jnp.zeros_like(rot_scr)
    lane = lax.broadcasted_iota(jnp.int32, (1, LANES), 1)
    spot = lax.rem(lane, half).astype(F32)
    position = len_ref[0].astype(F32)
    angles = position * jnp.exp(spot * (-jnp.log(jnp.full((1, LANES), ROTARY_BASE, F32)) / half))
    cos_row, sin_row = jnp.cos(angles), jnp.sin(angles)

    def rotate(v):
        turned = jnp.where(
            lane < half,
            -pltpu.roll(v, LANES - half, 1),
            pltpu.roll(v, half, 1),
        )
        return jnp.where(lane < R, v * cos_row + turned * sin_row, 0.0)

    ready("tok", "gains")
    x = tok[...].astype(F32)
    nrm[...] = (x * inv_rms(x) * gains[0:1, :]).astype(BF16)
    rows = lax.broadcasted_iota(jnp.int32, (G, 1), 0)
    fold(tok_row, jnp.sum(jnp.where(rows == me, x, 0.0), axis=0, keepdims=True))
    for j in range(3):
        fold(gain_f.at[j], gains[j + 1 : j + 2, :])

    q_nope = jnp.zeros((G, H * N), F32)
    q_rot = jnp.zeros((G, H * R), F32)
    lat_cols = jnp.zeros((G, CC), F32)
    for k in range(SPLIT):
        for copy in projection_loads(k):
            copy.wait()
        if k == SPLIT // 2:
            for copy in loads[8:]:
                copy.start()
        at = slice(k * part, (k + 1) * part)
        q_nope = q_nope + jnp.dot(nrm[:, at], wq[at, :], preferred_element_type=F32)
        q_rot = q_rot + jnp.dot(nrm[:, at], wqr[at, :], preferred_element_type=F32)
        lat_cols = lat_cols + jnp.dot(nrm[:, at], wld[at, :], preferred_element_type=F32)
    q_nope = q_nope.astype(BF16)
    ready("wku")
    for h in range(H):
        ql = jnp.dot(q_nope[:, h * N : (h + 1) * N], wku[h], preferred_element_type=F32)
        for t in range(G):
            qs_f[t, h : h + 1, 0:C] = ql[t : t + 1, :]
    rot_scr[:, 0 : H * R] = q_rot
    for h in range(H):
        start = h * R // LANES * LANES
        piece = rot_scr[:, start : start + LANES]
        if h * R % LANES:
            piece = pltpu.roll(piece, LANES - h * R % LANES, 1)
        piece = jnp.where(lane < R, piece, 0.0)
        for t in range(G):
            qs_f[t, h : h + 1, C : C + LANES] = piece[t : t + 1, :]
    for t in range(G):
        qs_f[t, 0:1, C + LANES : C + LANES + CC] = lat_cols[t : t + 1, :]
    for t in range(T):
        qs[t] = qs_f[t].astype(BF16)

    pl.semaphore_wait(barrier, T - 1 + E - 1)
    scatter("tp", me, T, qs, qrx, s1, r1)
    qrx[me] = qs[me]

    ready("wrd", "lgain", "cl", "cr")
    rot_scr[...] = jnp.zeros_like(rot_scr)
    rot_scr[:, 0:R] = lax.dot_general(nrm[...], wrd[...], NT, preferred_element_type=F32)
    raw = jnp.sum(jnp.where(rows == me, rot_scr[:, 0:LANES], 0.0), axis=0, keepdims=True)
    rope_new = rotate(raw.astype(BF16).astype(F32)).astype(BF16)
    rope_out_ref[...] = rope_new[:, 0:R]

    collect("tp", me, T, qs, qrx, s1, r1)
    for s in range(T):
        q_f[s * H : (s + 1) * H, :] = qrx[s].astype(F32)
        lat_f[:, s * CC : (s + 1) * CC] = q_f[s * H : s * H + 1, C + LANES : C + LANES + CC]
    lat = lat_f[...]
    lat_new = (lat * inv_rms(lat) * lgain[...]).astype(BF16)
    latent_out_ref[...] = lat_new
    lat_new_f = lat_new.astype(F32)

    q_lat = q_f[:, 0:C]
    q_pe = rotate(q_f[:, C : C + LANES]).astype(BF16)
    q_lat_b = q_lat.astype(BF16)
    scale = (N + R) ** (-0.5)
    pos_chunk = min(256, POS)
    q_pe_b = q_pe[:, 0:R]

    def score_step(p, carry):
        at = pl.ds(pl.multiple_of(p * pos_chunk, pos_chunk), pos_chunk)
        sc_scr[:, at] = lax.dot_general(
            q_lat_b, cl[0, at, :], NT, preferred_element_type=F32
        ) + jnp.dot(q_pe_b, cr[0, :, at], preferred_element_type=F32)
        return carry

    lax.fori_loop(0, POS // pos_chunk, score_step, 0)
    own_score = (
        jnp.sum(q_lat * lat_new_f, axis=-1, keepdims=True)
        + jnp.sum(q_pe.astype(F32) * rope_new.astype(F32), axis=-1, keepdims=True)
    ) * scale
    scores = sc_scr[...] * scale
    visible = lax.broadcasted_iota(jnp.int32, scores.shape, 1) < len_ref[0]
    row_max = jnp.maximum(
        jnp.max(jnp.where(visible, scores, -jnp.inf), axis=-1, keepdims=True), own_score
    )
    exps = jnp.where(visible, jnp.exp(scores - row_max), 0.0)
    own_exp = jnp.exp(own_score - row_max)
    denominator = jnp.sum(exps, axis=-1, keepdims=True) + own_exp
    probs = (exps / denominator).astype(BF16)
    own_prob = (own_exp / denominator).astype(BF16).astype(F32)
    lat_f[...] = lat_new_f
    lat_chunk = min(256, C)

    def attend_step(c, carry):
        at = pl.ds(pl.multiple_of(c * lat_chunk, lat_chunk), lat_chunk)
        att_f[:, at] = (
            jnp.dot(probs, cl[0, :, at], preferred_element_type=F32) + own_prob * lat_f[:, at]
        )
        return carry

    lax.fori_loop(0, C // lat_chunk, attend_step, 0)
    for s in range(T):
        as_[s] = att_f[s * H : (s + 1) * H, :].astype(BF16)
    scatter("tp", me, T, as_, arx, s2, r2)
    arx[me] = as_[me]
    ready("wvu", "wo")
    collect("tp", me, T, as_, arx, s2, r2)

    for t in range(T):
        block = arx[t].astype(F32)
        for h in range(H):
            st[h, t : t + 1, :] = block[h : h + 1, :]
    for h in range(H):
        val[:, h * V : (h + 1) * V] = jnp.dot(
            st[h].astype(BF16), wvu[h], preferred_element_type=F32
        ).astype(BF16)
    width = D // FOLD
    for j in range(FOLD):
        part_out = jnp.dot(
            val[...], wo[:, j * width : (j + 1) * width], preferred_element_type=F32
        )
        for t in range(G):
            ms_f[t, j : j + 1, :] = part_out[t : t + 1, :]
    for t in range(G):
        ms[t] = ms_f[t].astype(BF16)
    scatter("tp", me, T, ms, mrx, s3, r3)
    mrx[me] = ms[me]
    collect("tp", me, T, ms, mrx, s3, r3)
    mixed = mrx[0].astype(F32)
    for s in range(1, T):
        mixed = mixed + mrx[s].astype(F32)
    resid = tok_row[...] + mixed * folded_inv_rms(mixed) * gain_f[0]
    resid = resid.astype(BF16).astype(F32)
    tok_row[...] = resid
    expert_in = (resid * folded_inv_rms(resid) * gain_f[1]).astype(BF16)
    es[...] = expert_in
    scatter("ep", grp, E, es, erx, s4, r4)
    erx[grp] = expert_in
    collect("ep", grp, E, es, erx, s4, r4)
    for e in range(E):
        row = erx[e].astype(F32)
        for j in range(FOLD):
            xs_f[e : e + 1, j * width : (j + 1) * width] = row[j : j + 1, :]
    xs[...] = xs_f[...].astype(BF16)
    scatter("tp", me, T, xs, xrx, s5, r5)
    xrx[me] = xs[...]
    ready("wg", "wu", "wd")
    collect("tp", me, T, xs, xrx, s5, r5)
    for s in range(T):
        x_f[s * E : (s + 1) * E, :] = xrx[s].astype(F32)
    x_b[...] = x_f[...].astype(BF16)

    F = wg.shape[2]
    gate = mm_k(x_b, wg.at[0], F)
    up = mm_k(x_b, wu.at[0], F)
    hidden = (gate / (1.0 + jnp.exp(-gate)) * up).astype(BF16)

    out_chunk = min(1024, D)

    def down_step(n, carry):
        at = pl.ds(pl.multiple_of(n * out_chunk, out_chunk), out_chunk)
        x_f[:, at] = jnp.dot(hidden, wd[0, :, at], preferred_element_type=F32)
        return carry

    lax.fori_loop(0, D // out_chunk, down_step, 0)
    for s in range(T):
        ys[s] = x_f[s * E : (s + 1) * E, :].astype(BF16)
    scatter("tp", me, T, ys, yrx, s6, r6)
    yrx[me] = ys[me]
    collect("tp", me, T, ys, yrx, s6, r6)
    total = yrx[0].astype(F32)
    for s in range(1, T):
        total = total + yrx[s].astype(F32)
    for e in range(E):
        fold(tot_f, total[e : e + 1, :])
        rs[e] = tot_f[...].astype(BF16)
    scatter("ep", grp, E, rs, rrx, s7, r7)
    rrx[grp] = rs[grp]
    collect("ep", grp, E, rs, rrx, s7, r7)
    routed = jnp.zeros((FOLD, width), F32)
    for e in range(E):
        weight = jnp.float32(0.0)
        for k in range(routes_ref.shape[0]):
            weight = weight + jnp.where(routes_ref[k, me] == e, weights_ref[k, me], 0.0)
        routed = routed + weight * rrx[e].astype(F32)
    out = tok_row[...] + routed * folded_inv_rms(routed) * gain_f[2]
    for j in range(FOLD):
        out_row[:, j * width : (j + 1) * width] = out[j : j + 1, :]
    hidden_ref[...] = out_row[...].astype(BF16)

    drain("tp", me, T, qs, qrx, s1, r1)
    drain("tp", me, T, as_, arx, s2, r2)
    drain("tp", me, T, ms, mrx, s3, r3)
    drain("ep", grp, E, es, erx, s4, r4)
    drain("tp", me, T, xs, xrx, s5, r5)
    drain("tp", me, T, ys, yrx, s6, r6)
    drain("ep", grp, E, rs, rrx, s7, r7)


def on_device(
    tokens,
    norm_gains,
    w_query,
    w_query_rope,
    w_key_up,
    w_value_up,
    w_output,
    w_latent_down,
    latent_gain,
    w_rope_down,
    cache_latent,
    cache_rope,
    lengths,
    routes,
    route_weights,
    w_gate,
    w_up,
    w_down,
):
    T = lax.axis_size("tp")
    E = lax.axis_size("ep")
    G, D = tokens.shape
    H, N, C = w_key_up.shape
    V = w_value_up.shape[2]
    R = w_rope_down.shape[1]
    CC = w_latent_down.shape[1]
    POS = cache_latent.shape[1]
    W = C + LANES + round_up(CC, LANES)
    loaded = (
        tokens,
        norm_gains,
        w_query,
        w_key_up,
        w_query_rope,
        w_latent_down,
        w_rope_down.T,
        latent_gain.reshape(1, -1),
        cache_latent,
        jnp.swapaxes(cache_rope, 1, 2),
        w_value_up,
        w_output,
        w_gate,
        w_up,
        w_down,
    )
    sem = pltpu.SemaphoreType.DMA
    scratch = [pltpu.VMEM(a.shape, a.dtype) for a in loaded] + [
        pltpu.VMEM((G, D), BF16),
        pltpu.VMEM((G, round_up(H * R, LANES)), F32),
        pltpu.VMEM((T, H, W), F32),
        pltpu.VMEM((T, H, W), BF16),
        pltpu.VMEM((T, H, W), BF16),
        pltpu.VMEM((T * H, W), F32),
        pltpu.VMEM((1, C), F32),
        pltpu.VMEM((T * H, POS), F32),
        pltpu.VMEM((T * H, C), F32),
        pltpu.VMEM((T, H, C), BF16),
        pltpu.VMEM((T, H, C), BF16),
        pltpu.VMEM((H, G, C), F32),
        pltpu.VMEM((G, H * V), BF16),
        pltpu.VMEM((T, FOLD, D // FOLD), BF16),
        pltpu.VMEM((T, FOLD, D // FOLD), BF16),
        pltpu.VMEM((FOLD, D // FOLD), F32),
        pltpu.VMEM((FOLD, D // FOLD), BF16),
        pltpu.VMEM((E, FOLD, D // FOLD), BF16),
        pltpu.VMEM((E, D), F32),
        pltpu.VMEM((E, D), BF16),
        pltpu.VMEM((T, E, D), BF16),
        pltpu.VMEM((T * E, D), F32),
        pltpu.VMEM((T * E, D), BF16),
        pltpu.VMEM((T, E, D), BF16),
        pltpu.VMEM((T, E, D), BF16),
        pltpu.VMEM((E, FOLD, D // FOLD), BF16),
        pltpu.VMEM((E, FOLD, D // FOLD), BF16),
        pltpu.VMEM((T, FOLD, D // FOLD), F32),
        pltpu.VMEM((3, FOLD, D // FOLD), F32),
        pltpu.VMEM((1, D), F32),
        pltpu.VMEM((FOLD, D // FOLD), F32),
        sem((len(loaded),)),
        sem((len(loaded), SPLIT)),
        sem((T,)),
        sem((T,)),
        sem((T,)),
        sem((T,)),
        sem((T,)),
        sem((T,)),
        sem((E,)),
        sem((E,)),
        sem((T,)),
        sem((T,)),
        sem((T,)),
        sem((T,)),
        sem((E,)),
        sem((E,)),
    ]
    smem = pl.BlockSpec(memory_space=pltpu.SMEM)
    vmem = pl.BlockSpec(memory_space=pltpu.VMEM)
    anywhere = pl.BlockSpec(memory_space=pl.ANY)
    return pl.pallas_call(
        layer_kernel,
        out_shape=(
            jax.ShapeDtypeStruct((1, D), BF16),
            jax.ShapeDtypeStruct((1, C), BF16),
            jax.ShapeDtypeStruct((1, R), BF16),
        ),
        in_specs=[smem] * 3 + [anywhere] * len(loaded),
        out_specs=(vmem,) * 3,
        scratch_shapes=scratch,
        compiler_params=pltpu.CompilerParams(
            collective_id=0, has_side_effects=True, vmem_limit_bytes=60 * 1024 * 1024
        ),
    )(lengths, routes.T, route_weights.T, *loaded)


def solution(mesh):
    in_specs = (
        P("ep", None),
        P(),
        P(None, "tp"),
        P(None, "tp"),
        P("tp", None, None),
        P("tp", None, None),
        P("tp", None),
        P(None, "tp"),
        P(),
        P(),
        P(("ep", "tp"), None, None),
        P(("ep", "tp"), None, None),
        P(("ep", "tp")),
        P("ep", None),
        P("ep", None),
        P("ep", None, "tp"),
        P("ep", None, "tp"),
        P("ep", "tp", None),
    )
    out_specs = (P(("ep", "tp"), None), P(("ep", "tp"), None), P(("ep", "tp"), None))
    return jax.shard_map(
        on_device, mesh=mesh, in_specs=in_specs, out_specs=out_specs, check_vma=False
    )
```

```python
import functools
import jax
import jax.numpy as jnp
from jax import lax
from jax.experimental import pallas as pl
from jax.experimental.pallas import tpu as pltpu
from jax.sharding import PartitionSpec as P

EPSILON = 1e-06
ROTARY_BASE = 500000.0
LANES = 128
FOLD = 8
SPLIT = 4
F32 = jnp.float32
BF16 = jnp.bfloat16


def round_up(value, step):
    return (value + step - 1) // step * step


def inv_rms(v):
    return lax.rsqrt(jnp.mean(v * v, axis=-1, keepdims=True) + EPSILON)


def folded_inv_rms(v):
    lanes = jnp.sum(v * v, axis=0, keepdims=True)
    mean = jnp.sum(lanes, axis=1, keepdims=True) / (v.shape[0] * v.shape[1])
    return lax.rsqrt(mean + EPSILON)


def fold(dst, row):
    width = row.shape[1] // FOLD
    for j in range(FOLD):
        dst[j : j + 1, :] = row[:, j * width : (j + 1) * width]


def layer_kernel(
    len_ref,
    routes_ref,
    weights_ref,
    *refs,
):
    hbm = refs[:15]
    hidden_ref, latent_out_ref, rope_out_ref = refs[15:18]
    vm = refs[18:33]
    (
        nrm,
        rot_scr,
        qs_f,
        qs,
        qrx,
        q_f,
        lat_f,
        sc_scr,
        att_f,
        as_,
        arx,
        st,
        val,
        ms,
        mrx,
        tok_row,
        es,
        erx,
        xs_f,
        xs,
        xrx,
        x_f,
        x_b,
        ys,
        yrx,
        rs,
        rrx,
        ms_f,
        gain_f,
        out_row,
        tot_f,
        load_sem,
        part_sem,
        s1,
        r1,
        s2,
        r2,
        s3,
        r3,
        s4,
        r4,
        s5,
        r5,
        s6,
        r6,
        s7,
        r7,
    ) = refs[33:]
    tok, gains, wq, wku, wqr, wld, wrd, lgain, cl, cr, wvu, wo, wg, wu, wd = vm
    T = lax.axis_size("tp")
    E = lax.axis_size("ep")
    me = lax.axis_index("tp")
    grp = lax.axis_index("ep")
    G, D = tok.shape
    H, N, C = wku.shape
    V = wvu.shape[2]
    R = wrd.shape[0]
    CC = wld.shape[1]
    POS = cl.shape[1]
    half = R // 2
    NT = (((1,), (1,)), ((), ()))

    barrier = pltpu.get_barrier_semaphore()

    def greet_tp(i, carry):
        pl.semaphore_signal(
            barrier,
            inc=1,
            device_id={"tp": lax.rem(me + i, T)},
            device_id_type=pl.DeviceIdType.MESH,
        )
        return carry

    def greet_ep(i, carry):
        pl.semaphore_signal(
            barrier,
            inc=1,
            device_id={"ep": lax.rem(grp + i, E)},
            device_id_type=pl.DeviceIdType.MESH,
        )
        return carry

    lax.fori_loop(1, T, greet_tp, 0)
    lax.fori_loop(1, E, greet_ep, 0)

    loads = [pltpu.make_async_copy(hbm[i], vm[i], load_sem.at[i]) for i in range(15)]
    part = D // SPLIT

    def projection_loads(k):
        at = pl.ds(k * part, part)
        return [
            pltpu.make_async_copy(hbm[i].at[at], vm[i].at[at], part_sem.at[i, k])
            for i in (2, 4, 5)
        ]

    for i in (0, 1):
        loads[i].start()
    for k in range(SPLIT):
        for copy in projection_loads(k):
            copy.start()
    for i in (3, 6, 7):
        loads[i].start()
    names = (
        ("tok", "gains", "wq", "wku", "wqr", "wld", "wrd", "lgain")
        + ("cl", "cr", "wvu", "wo", "wg", "wu", "wd")
    )

    def ready(*which):
        for name in which:
            loads[names.index(name)].wait()

    def rdma(axis, src, dst, send, recv, peer):
        return pltpu.make_async_remote_copy(
            src_ref=src,
            dst_ref=dst,
            send_sem=send,
            recv_sem=recv,
            device_id={axis: peer},
            device_id_type=pl.DeviceIdType.MESH,
        )

    def scatter(axis, mine, size, src, dst, send, recv):
        def pick(peer):
            return src.at[peer] if len(src.shape) == len(dst.shape) else src

        def go(i, carry):
            peer = lax.rem(mine + i, size)
            rdma(axis, pick(peer), dst.at[mine], send.at[peer], recv.at[mine], peer).start()
            return carry

        lax.fori_loop(1, size, go, 0)

    def collect(axis, mine, size, src, dst, send, recv):
        def pick(peer):
            return src.at[peer] if len(src.shape) == len(dst.shape) else src

        def go(i, carry):
            peer = lax.rem(mine + i, size)
            copy = rdma(axis, pick(peer), dst.at[peer], send.at[peer], recv.at[peer], peer)
            copy.wait_recv()
            return carry

        lax.fori_loop(1, size, go, 0)

    def drain(axis, mine, size, src, dst, send, recv):
        def pick(peer):
            return src.at[peer] if len(src.shape) == len(dst.shape) else src

        def go(i, carry):
            peer = lax.rem(mine + i, size)
            copy = rdma(axis, pick(peer), dst.at[peer], send.at[peer], recv.at[peer], peer)
            copy.wait_send()
            return carry

        lax.fori_loop(1, size, go, 0)

    def mm_k(x_ref, w_ref, width):
        chunk = min(1024, x_ref.shape[1])

        def step(k, acc):
            at = pl.ds(pl.multiple_of(k * chunk, chunk), chunk)
            return acc + jnp.dot(x_ref[:, at], w_ref[at, :], preferred_element_type=F32)

        return lax.fori_loop(
            0, x_ref.shape[1] // chunk, step, jnp.zeros((x_ref.shape[0], width), F32)
        )

    qs_f[...] = jnp.zeros_like(qs_f)
    rot_scr[...] = jnp.zeros_like(rot_scr)
    lane = lax.broadcasted_iota(jnp.int32, (1, LANES), 1)
    spot = lax.rem(lane, half).astype(F32)
    position = len_ref[0].astype(F32)
    angles = position * jnp.exp(spot * (-jnp.log(jnp.full((1, LANES), ROTARY_BASE, F32)) / half))
    cos_row, sin_row = jnp.cos(angles), jnp.sin(angles)

    def rotate(v):
        turned = jnp.where(
            lane < half,
            -pltpu.roll(v, LANES - half, 1),
            pltpu.roll(v, half, 1),
        )
        return jnp.where(lane < R, v * cos_row + turned * sin_row, 0.0)

    ready("tok", "gains")
    x = tok[...].astype(F32)
    nrm[...] = (x * inv_rms(x) * gains[0:1, :]).astype(BF16)
    rows = lax.broadcasted_iota(jnp.int32, (G, 1), 0)
    fold(tok_row, jnp.sum(jnp.where(rows == me, x, 0.0), axis=0, keepdims=True))
    for j in range(3):
        fold(gain_f.at[j], gains[j + 1 : j + 2, :])

    q_nope = jnp.zeros((G, H * N), F32)
    q_rot = jnp.zeros((G, H * R), F32)
    lat_cols = jnp.zeros((G, CC), F32)
    for k in range(SPLIT):
        for copy in projection_loads(k):
            copy.wait()
        if k == SPLIT // 2:
            for copy in loads[8:]:
                copy.start()
        at = slice(k * part, (k + 1) * part)
        q_nope = q_nope + jnp.dot(nrm[:, at], wq[at, :], preferred_element_type=F32)
        q_rot = q_rot + jnp.dot(nrm[:, at], wqr[at, :], preferred_element_type=F32)
        lat_cols = lat_cols + jnp.dot(nrm[:, at], wld[at, :], preferred_element_type=F32)
    q_nope = q_nope.astype(BF16)
    ready("wku")
    for h in range(H):
        ql = jnp.dot(q_nope[:, h * N : (h + 1) * N], wku[h], preferred_element_type=F32)
        for t in range(G):
            qs_f[t, h : h + 1, 0:C] = ql[t : t + 1, :]
    rot_scr[:, 0 : H * R] = q_rot
    for h in range(H):
        start = h * R // LANES * LANES
        piece = rot_scr[:, start : start + LANES]
        if h * R % LANES:
            piece = pltpu.roll(piece, LANES - h * R % LANES, 1)
        piece = jnp.where(lane < R, piece, 0.0)
        for t in range(G):
            qs_f[t, h : h + 1, C : C + LANES] = piece[t : t + 1, :]
    for t in range(G):
        qs_f[t, 0:1, C + LANES : C + LANES + CC] = lat_cols[t : t + 1, :]
    for t in range(T):
        qs[t] = qs_f[t].astype(BF16)

    pl.semaphore_wait(barrier, T - 1 + E - 1)
    scatter("tp", me, T, qs, qrx, s1, r1)
    qrx[me] = qs[me]

    ready("wrd", "lgain", "cl", "cr")
    rot_scr[...] = jnp.zeros_like(rot_scr)
    rot_scr[:, 0:R] = lax.dot_general(nrm[...], wrd[...], NT, preferred_element_type=F32)
    raw = jnp.sum(jnp.where(rows == me, rot_scr[:, 0:LANES], 0.0), axis=0, keepdims=True)
    rope_new = rotate(raw.astype(BF16).astype(F32)).astype(BF16)
    rope_out_ref[...] = rope_new[:, 0:R]

    collect("tp", me, T, qs, qrx, s1, r1)
    for s in range(T):
        q_f[s * H : (s + 1) * H, :] = qrx[s].astype(F32)
        lat_f[:, s * CC : (s + 1) * CC] = q_f[s * H : s * H + 1, C + LANES : C + LANES + CC]
    lat = lat_f[...]
    lat_new = (lat * inv_rms(lat) * lgain[...]).astype(BF16)
    latent_out_ref[...] = lat_new
    lat_new_f = lat_new.astype(F32)

    q_lat = q_f[:, 0:C]
    q_pe = rotate(q_f[:, C : C + LANES]).astype(BF16)
    q_lat_b = q_lat.astype(BF16)
    scale = (N + R) ** (-0.5)
    pos_chunk = min(256, POS)
    q_pe_b = q_pe[:, 0:R]

    def score_step(p, carry):
        at = pl.ds(pl.multiple_of(p * pos_chunk, pos_chunk), pos_chunk)
        sc_scr[:, at] = lax.dot_general(
            q_lat_b, cl[0, at, :], NT, preferred_element_type=F32
        ) + jnp.dot(q_pe_b, cr[0, :, at], preferred_element_type=F32)
        return carry

    lax.fori_loop(0, POS // pos_chunk, score_step, 0)
    own_score = (
        jnp.sum(q_lat * lat_new_f, axis=-1, keepdims=True)
        + jnp.sum(q_pe.astype(F32) * rope_new.astype(F32), axis=-1, keepdims=True)
    ) * scale
    scores = sc_scr[...] * scale
    visible = lax.broadcasted_iota(jnp.int32, scores.shape, 1) < len_ref[0]
    row_max = jnp.maximum(
        jnp.max(jnp.where(visible, scores, -jnp.inf), axis=-1, keepdims=True), own_score
    )
    exps = jnp.where(visible, jnp.exp(scores - row_max), 0.0)
    own_exp = jnp.exp(own_score - row_max)
    denominator = jnp.sum(exps, axis=-1, keepdims=True) + own_exp
    probs = (exps / denominator).astype(BF16)
    own_prob = (own_exp / denominator).astype(BF16).astype(F32)
    lat_f[...] = lat_new_f
    lat_chunk = min(256, C)

    def attend_step(c, carry):
        at = pl.ds(pl.multiple_of(c * lat_chunk, lat_chunk), lat_chunk)
        att_f[:, at] = (
            jnp.dot(probs, cl[0, :, at], preferred_element_type=F32) + own_prob * lat_f[:, at]
        )
        return carry

    lax.fori_loop(0, C // lat_chunk, attend_step, 0)
    for s in range(T):
        as_[s] = att_f[s * H : (s + 1) * H, :].astype(BF16)
    scatter("tp", me, T, as_, arx, s2, r2)
    arx[me] = as_[me]
    ready("wvu", "wo")
    collect("tp", me, T, as_, arx, s2, r2)

    for t in range(T):
        block = arx[t].astype(F32)
        for h in range(H):
            st[h, t : t + 1, :] = block[h : h + 1, :]
    for h in range(H):
        val[:, h * V : (h + 1) * V] = jnp.dot(
            st[h].astype(BF16), wvu[h], preferred_element_type=F32
        ).astype(BF16)
    width = D // FOLD
    for j in range(FOLD):
        part_out = jnp.dot(
            val[...], wo[:, j * width : (j + 1) * width], preferred_element_type=F32
        )
        for t in range(G):
            ms_f[t, j : j + 1, :] = part_out[t : t + 1, :]
    for t in range(G):
        ms[t] = ms_f[t].astype(BF16)
    scatter("tp", me, T, ms, mrx, s3, r3)
    mrx[me] = ms[me]
    collect("tp", me, T, ms, mrx, s3, r3)
    mixed = mrx[0].astype(F32)
    for s in range(1, T):
        mixed = mixed + mrx[s].astype(F32)
    resid = tok_row[...] + mixed * folded_inv_rms(mixed) * gain_f[0]
    resid = resid.astype(BF16).astype(F32)
    tok_row[...] = resid
    expert_in = (resid * folded_inv_rms(resid) * gain_f[1]).astype(BF16)
    es[...] = expert_in
    scatter("ep", grp, E, es, erx, s4, r4)
    erx[grp] = expert_in
    collect("ep", grp, E, es, erx, s4, r4)
    for e in range(E):
        row = erx[e].astype(F32)
        for j in range(FOLD):
            xs_f[e : e + 1, j * width : (j + 1) * width] = row[j : j + 1, :]
    xs[...] = xs_f[...].astype(BF16)
    scatter("tp", me, T, xs, xrx, s5, r5)
    xrx[me] = xs[...]
    ready("wg", "wu", "wd")
    collect("tp", me, T, xs, xrx, s5, r5)
    for s in range(T):
        x_f[s * E : (s + 1) * E, :] = xrx[s].astype(F32)
    x_b[...] = x_f[...].astype(BF16)

    F = wg.shape[2]
    gate = mm_k(x_b, wg.at[0], F)
    up = mm_k(x_b, wu.at[0], F)
    hidden = (gate / (1.0 + jnp.exp(-gate)) * up).astype(BF16)

    out_chunk = min(1024, D)

    def down_step(n, carry):
        at = pl.ds(pl.multiple_of(n * out_chunk, out_chunk), out_chunk)
        x_f[:, at] = jnp.dot(hidden, wd[0, :, at], preferred_element_type=F32)
        return carry

    lax.fori_loop(0, D // out_chunk, down_step, 0)
    for s in range(T):
        ys[s] = x_f[s * E : (s + 1) * E, :].astype(BF16)
    scatter("tp", me, T, ys, yrx, s6, r6)
    yrx[me] = ys[me]
    collect("tp", me, T, ys, yrx, s6, r6)
    total = yrx[0].astype(F32)
    for s in range(1, T):
        total = total + yrx[s].astype(F32)
    for e in range(E):
        fold(tot_f, total[e : e + 1, :])
        rs[e] = tot_f[...].astype(BF16)
    scatter("ep", grp, E, rs, rrx, s7, r7)
    rrx[grp] = rs[grp]
    collect("ep", grp, E, rs, rrx, s7, r7)
    routed = jnp.zeros((FOLD, width), F32)
    for e in range(E):
        weight = jnp.float32(0.0)
        for k in range(routes_ref.shape[0]):
            weight = weight + jnp.where(routes_ref[k, me] == e, weights_ref[k, me], 0.0)
        routed = routed + weight * rrx[e].astype(F32)
    out = tok_row[...] + routed * folded_inv_rms(routed) * gain_f[2]
    for j in range(FOLD):
        out_row[:, j * width : (j + 1) * width] = out[j : j + 1, :]
    hidden_ref[...] = out_row[...].astype(BF16)

    drain("tp", me, T, qs, qrx, s1, r1)
    drain("tp", me, T, as_, arx, s2, r2)
    drain("tp", me, T, ms, mrx, s3, r3)
    drain("ep", grp, E, es, erx, s4, r4)
    drain("tp", me, T, xs, xrx, s5, r5)
    drain("tp", me, T, ys, yrx, s6, r6)
    drain("ep", grp, E, rs, rrx, s7, r7)


def hand_over(*refs):
    count = len(refs) // 2
    for source, target in zip(refs[:count], refs[count:]):
        target[...] = source[...]


def on_device(
    tokens,
    norm_gains,
    w_query,
    w_query_rope,
    w_key_up,
    w_value_up,
    w_output,
    w_latent_down,
    latent_gain,
    w_rope_down,
    cache_latent,
    cache_rope,
    lengths,
    routes,
    route_weights,
    w_gate,
    w_up,
    w_down,
):
    T = lax.axis_size("tp")
    E = lax.axis_size("ep")
    G, D = tokens.shape
    H, N, C = w_key_up.shape
    V = w_value_up.shape[2]
    R = w_rope_down.shape[1]
    CC = w_latent_down.shape[1]
    POS = cache_latent.shape[1]
    W = C + LANES + round_up(CC, LANES)
    loaded = (
        tokens,
        norm_gains,
        w_query,
        w_key_up,
        w_query_rope,
        w_latent_down,
        w_rope_down.T,
        latent_gain.reshape(1, -1),
        cache_latent,
        jnp.swapaxes(cache_rope, 1, 2),
        w_value_up,
        w_output,
        w_gate,
        w_up,
        w_down,
    )
    sem = pltpu.SemaphoreType.DMA
    scratch = [pltpu.VMEM(a.shape, a.dtype) for a in loaded] + [
        pltpu.VMEM((G, D), BF16),
        pltpu.VMEM((G, round_up(H * R, LANES)), F32),
        pltpu.VMEM((T, H, W), F32),
        pltpu.VMEM((T, H, W), BF16),
        pltpu.VMEM((T, H, W), BF16),
        pltpu.VMEM((T * H, W), F32),
        pltpu.VMEM((1, C), F32),
        pltpu.VMEM((T * H, POS), F32),
        pltpu.VMEM((T * H, C), F32),
        pltpu.VMEM((T, H, C), BF16),
        pltpu.VMEM((T, H, C), BF16),
        pltpu.VMEM((H, G, C), F32),
        pltpu.VMEM((G, H * V), BF16),
        pltpu.VMEM((T, FOLD, D // FOLD), BF16),
        pltpu.VMEM((T, FOLD, D // FOLD), BF16),
        pltpu.VMEM((FOLD, D // FOLD), F32),
        pltpu.VMEM((FOLD, D // FOLD), BF16),
        pltpu.VMEM((E, FOLD, D // FOLD), BF16),
        pltpu.VMEM((E, D), F32),
        pltpu.VMEM((E, D), BF16),
        pltpu.VMEM((T, E, D), BF16),
        pltpu.VMEM((T * E, D), F32),
        pltpu.VMEM((T * E, D), BF16),
        pltpu.VMEM((T, E, D), BF16),
        pltpu.VMEM((T, E, D), BF16),
        pltpu.VMEM((E, FOLD, D // FOLD), BF16),
        pltpu.VMEM((E, FOLD, D // FOLD), BF16),
        pltpu.VMEM((T, FOLD, D // FOLD), F32),
        pltpu.VMEM((3, FOLD, D // FOLD), F32),
        pltpu.VMEM((1, D), F32),
        pltpu.VMEM((FOLD, D // FOLD), F32),
        sem((len(loaded),)),
        sem((len(loaded), SPLIT)),
        sem((T,)),
        sem((T,)),
        sem((T,)),
        sem((T,)),
        sem((T,)),
        sem((T,)),
        sem((E,)),
        sem((E,)),
        sem((T,)),
        sem((T,)),
        sem((T,)),
        sem((T,)),
        sem((E,)),
        sem((E,)),
    ]
    smem = pl.BlockSpec(memory_space=pltpu.SMEM)
    vmem = pl.BlockSpec(memory_space=pltpu.VMEM)
    anywhere = pl.BlockSpec(memory_space=pl.ANY)
    shapes = tuple(jax.ShapeDtypeStruct((1, n), BF16) for n in (D, C, R))
    results = pl.pallas_call(
        layer_kernel,
        out_shape=shapes,
        in_specs=[smem] * 3 + [anywhere] * len(loaded),
        out_specs=(vmem,) * 3,
        scratch_shapes=scratch,
        compiler_params=pltpu.CompilerParams(
            collective_id=0, has_side_effects=True, vmem_limit_bytes=60 * 1024 * 1024
        ),
    )(lengths, routes.T, route_weights.T, *loaded)
    return pl.pallas_call(
        hand_over, out_shape=shapes, in_specs=[vmem] * 3, out_specs=(vmem,) * 3
    )(*results)


def solution(mesh):
    in_specs = (
        P("ep", None),
        P(),
        P(None, "tp"),
        P(None, "tp"),
        P("tp", None, None),
        P("tp", None, None),
        P("tp", None),
        P(None, "tp"),
        P(),
        P(),
        P(("ep", "tp"), None, None),
        P(("ep", "tp"), None, None),
        P(("ep", "tp")),
        P("ep", None),
        P("ep", None),
        P("ep", None, "tp"),
        P("ep", None, "tp"),
        P("ep", "tp", None),
    )
    out_specs = (P(("ep", "tp"), None), P(("ep", "tp"), None), P(("ep", "tp"), None))
    return jax.shard_map(
        on_device, mesh=mesh, in_specs=in_specs, out_specs=out_specs, check_vma=False
    )
```
